32 devices in a mesh: ep: 8 (over z, x), tp: 4 (over y, core).
Axes of the slice: x: 2, y: 2, z: 4, core: 2. Of those that a mesh axis runs over, the one named last changes fastest.
Arguments:
- tokens: bfloat16 [4096, 4096], P('ep', 'tp'), may hold values from -60 to 60
- routes: int32 [4096, 4], P('ep'), may hold values from 0 to 31, all different within a row; in each aligned block of 512 rows (0 to 511, 512 to 1023, ...) at most 128 rows name the same one
- route_weights: float32 [4096, 4], P('ep'), may hold values from 0.1 to 1
- pre_gain: float32 [4096], P('tp'), may hold values from 0.1 to 1.9
- expert_gate: bfloat16 [32, 4096, 512], P('ep', 'tp'), may hold values from -0.09375 to 0.09375
- expert_up: bfloat16 [32, 4096, 512], P('ep', 'tp'), may hold values from -0.09375 to 0.09375
- expert_down: bfloat16 [32, 512, 4096], P('ep', None, 'tp'), may hold values from -1 to 1
- shared_gate: bfloat16 [4096, 512], P('tp'), may hold values from -0.09375 to 0.09375
- shared_up: bfloat16 [4096, 512], P('tp'), may hold values from -0.09375 to 0.09375
- shared_down: bfloat16 [512, 4096], P(None, 'tp'), may hold values from -1 to 1
- post_gain: float32 [4096], P('tp'), may hold values from 0.1 to 1.9
Outputs:
- layer_out: bfloat16 [4096, 4096], P('ep', 'tp')
The draws below stay inside these ranges and needn't reach their ends.
Inputs may be any that keep to these rules, and one draw needn't show every extreme that they name: `routes`: each row names 4 different experts. Within each aligned block of 512 rows (the tokens of one index of ep) no expert is named more than 128 times, a bound that some block reaches.
All inputs are finite; a program needn't handle non-finite values.
Results may differ from the reference program's by a relative error of at most 0.022.
Values may be sent and summed in bfloat16 or wider, within the bound.
No kernel may reach another device: no remote copies, remote signals or barrier semaphores. Data moves between devices by JAX's collectives and lax.ppermute only.
A program may use at most 128 MiB of HBM per device.

```python
import math
import jax
import jax.numpy as jnp
import numpy as np
from jax import lax

D = 4096
FF = 512
FS = 512
TOPK = 4
TOK_EP = 512
EXPERTS = 32
TOKENS = 4096
CAP = 128
N_EP = 8
N_TP = 4


def draw_tokens(key, part):
    key_base, key_rows, key_cols = jax.random.split(key, 3)
    ramp = 3.0 ** (jnp.arange(D, dtype=jnp.float32) / D)
    columns = ramp * jax.random.uniform(key_cols, (D,), jnp.float32, 0.5, 2.0)
    scales = jnp.exp(jax.random.uniform(key_rows, (TOKENS, 1), jnp.float32, -1.0, 1.0))
    base = jnp.clip(jax.random.normal(key_base, (TOKENS, D), jnp.float32), -6.0, 6.0)
    return jnp.clip(base * scales * columns, -60.0, 60.0).astype(jnp.bfloat16)


def ramped_weight(key, shape, fan_in):
    key_base, key_cols = jax.random.split(key)
    ramp = 3.0 ** (jnp.arange(D, dtype=jnp.float32) / D)
    columns = ramp * jax.random.uniform(key_cols, (D,), jnp.float32, 0.5, 2.0) / 2.0
    base = jnp.clip(jax.random.normal(key_base, shape, jnp.float32), -6.0, 6.0) * fan_in ** (-0.5)
    return jnp.clip(base * columns, -1.0, 1.0).astype(jnp.bfloat16)


def draw_expert_down(key, part):
    return ramped_weight(key, (EXPERTS, FF, D), FF)


def draw_shared_down(key, part):
    return ramped_weight(key, (FS, D), FS)


def steps_of(rng, dims, cuts, low, top_value):
    def one(position, shards_of):
        steps = jax.random.uniform(jax.random.fold_in(jax.random.fold_in(rng, 6), position), (shards_of,), jnp.float32, low / len(cuts), top_value / len(cuts))
        return jnp.repeat(jnp.exp(steps), dims[position] // shards_of).reshape((-1,) + (1,) * (len(dims) - position - 1))

    factor_of = one(*cuts[0])
    for cut in cuts[1:]:
        factor_of = factor_of * one(*cut)
    return factor_of


def routed_block(rng, own, number, rows, number_of, top, limit, slope):
    ranking = jax.random.permutation(rng, number_of)
    heavy_load, usual = shares(number_of, rows * top, limit, slope, True), shares(number_of, rows * top, limit, slope, False)
    places = jnp.arange(number_of)

    def named(sizes, offset_by):
        used = int((sizes > 0).sum())
        fixed = max(1, used // 4)
        moved = fixed + (places - fixed + offset_by * (used - fixed)) % max(1, number_of - fixed)
        return jnp.zeros((number_of,), jnp.int32).at[ranking[jnp.where(places < fixed, places, moved)]].set(jnp.asarray(sizes, jnp.int32))

    sizes = jnp.where(number % 4 == 0, named(heavy_load, number // 4), named(usual, number - number // 4 - 1))
    mixed = jax.random.permutation(jax.random.fold_in(own, 3), number_of)
    source_of, sink = mixed[0:number_of // 2 * 2:2], mixed[1:number_of // 2 * 2:2]
    slack = jnp.minimum(sizes[source_of] - 1, limit - sizes[sink]) // 2
    slack = jnp.where((source_of == ranking[0]) | (sink == ranking[0]) | (sizes[sink] == 0), 0, jnp.maximum(slack, 0))
    moved = jax.random.randint(jax.random.fold_in(own, 4), (number_of // 2,), 0, 1 << 20) % (slack + 1)
    sizes = sizes.at[source_of].add(-moved).at[sink].add(moved)
    labels = jnp.searchsorted(jnp.cumsum(sizes), jnp.arange(rows * top), side="right").astype(jnp.int32)
    table = labels.reshape(top, rows).T
    table = table[jax.random.permutation(jax.random.fold_in(own, 1), rows)]
    offset_by = jax.random.randint(jax.random.fold_in(own, 2), (rows, 1), 0, top)
    return jnp.take_along_axis(table, (jnp.arange(top)[None, :] + offset_by) % top, axis=1)


def shares(count, total, reach, lean, full):
    portions = [(1 << 20) // math.isqrt(grade ** lean) + 1 for grade in range(1, count + 1)]
    largest = reach if full else min(reach, max(-(-total // count), total * portions[0] // sum(portions)))
    least = 1 if total - largest >= count - 1 else 0
    counts, surplus = [largest] + [least] * (count - 1), total - largest - least * (count - 1)
    while surplus > 0:
        candidates = [i for i in range(1, count) if counts[i] < largest] or [i for i in range(1, count) if counts[i] < reach]
        mass, budget = sum([portions[i] for i in candidates]), surplus
        for i in candidates:
            extra = min(reach - counts[i], max(1, budget * portions[i] // mass), surplus)
            counts[i] = counts[i] + extra
            surplus = surplus - extra
    return np.array(counts)


def centred(rng, shape, width, reach, cuts=(), kind=jnp.bfloat16):
    gain = steps_of(rng, shape, cuts, -0.22, 0.18) if cuts else 1.0
    drawn = jax.random.normal(rng, shape, jnp.float32) * width * gain
    return jnp.minimum(jnp.maximum(drawn, -reach), reach).astype(kind)


def setup_inputs(seed: int = 0) -> dict:
    streams_of = jax.random.split(jax.random.key(seed), 12)
    tokens = draw_tokens(jax.random.fold_in(streams_of[11], 71), 0)
    routes_keys = jax.random.split(jax.random.fold_in(streams_of[1], 1), TOKENS // TOK_EP)
    routes_turns = jax.random.permutation(jax.random.fold_in(streams_of[1], 3), TOKENS // TOK_EP)
    routes = jax.vmap(lambda own, number: routed_block(jax.random.fold_in(streams_of[1], 2), own, number, TOK_EP, EXPERTS, TOPK, CAP, 2))(routes_keys, routes_turns).reshape((TOKENS, TOPK))
    route_weights = jnp.clip(jnp.exp(math.log(1.0) - 2.3025851 * jax.random.uniform(streams_of[2], (TOKENS, TOPK), jnp.float32) ** steps_of(streams_of[2], (TOKENS, TOPK), ((0, 8),), -0.2, 0.2)), 0.1, 1.0)
    pre_gain = jnp.clip(1.0 + 0.18 * jax.random.normal(streams_of[3], (D,), jnp.float32), 0.1, 1.9)
    expert_gate = centred(streams_of[4], (EXPERTS, D, FF), D ** -0.5, 0.09375, ((0, 8), (1, 4)))
    expert_up = centred(streams_of[5], (EXPERTS, D, FF), D ** -0.5, 0.09375, ((0, 8), (1, 4)))
    expert_down = draw_expert_down(jax.random.fold_in(streams_of[11], 71), 0)
    shared_gate = centred(streams_of[7], (D, FS), D ** -0.5, 0.09375, ((0, 4),))
    shared_up = centred(streams_of[8], (D, FS), D ** -0.5, 0.09375, ((0, 4),))
    shared_down = draw_shared_down(jax.random.fold_in(streams_of[11], 71), 0)
    post_gain = jnp.clip(1.0 + 0.18 * jax.random.normal(streams_of[10], (D,), jnp.float32), 0.1, 1.9)
    return {"tokens": tokens, "routes": routes, "route_weights": route_weights, "pre_gain": pre_gain, "expert_gate": expert_gate, "expert_up": expert_up, "expert_down": expert_down, "shared_gate": shared_gate, "shared_up": shared_up, "shared_down": shared_down, "post_gain": post_gain}


epsilon = 1e-06

def inverse_norm(values):
    return lax.rsqrt(lax.optimization_barrier(jnp.mean(values * values, axis=1)) + epsilon)

def blocked_product(inputs, weight):
    row_count = inputs.shape[0]
    out_width = weight.shape[1]
    pieces = inputs.reshape(row_count, N_TP, D // N_TP).astype(jnp.float32)
    blocks = weight.reshape(N_TP, D // N_TP, out_width).astype(jnp.float32)
    partial_value = jnp.einsum('rnd,ndf->nrf', pieces, blocks)
    rounded = lax.optimization_barrier(partial_value.astype(jnp.bfloat16))
    return lax.optimization_barrier(jnp.sum(rounded.astype(jnp.float32), axis=0))

def reference(tokens, routes, route_weights, pre_gain, expert_gate, expert_up, expert_down, shared_gate, shared_up, shared_down, post_gain):
    inputs = tokens.astype(jnp.float32)
    normed = (inputs * inverse_norm(inputs)[:, None] * pre_gain.astype(jnp.float32)).astype(jnp.bfloat16)
    per_block = TOK_EP * TOPK
    flat_ids = routes.reshape(N_EP, per_block).astype(jnp.int32)
    one_hot = (flat_ids[:, :, None] == jnp.arange(EXPERTS, dtype=jnp.int32)[None, None, :]).astype(jnp.int32)
    slots = lax.optimization_barrier(jnp.sum(jnp.cumsum(one_hot, axis=1) * one_hot, axis=2)) - 1
    sources = jnp.arange(N_EP, dtype=jnp.int32)[:, None]
    positions = (sources * CAP + slots).reshape(-1).astype(jnp.int32)
    token_index = (sources * TOK_EP + jnp.arange(per_block, dtype=jnp.int32)[None, :] // TOPK).reshape(-1).astype(jnp.int32)
    expert_index = flat_ids.reshape(-1)
    token_table = jnp.full((EXPERTS, N_EP * CAP), TOKENS, jnp.int32).at[expert_index, positions].set(token_index)
    weight_table = jnp.zeros((EXPERTS, N_EP * CAP), jnp.float32).at[expert_index, positions].set(route_weights.reshape(-1).astype(jnp.float32))

    def expert_step(totals, stacked):
        table_rows, table_weights, gate_weight, up_weight, down_weight = stacked
        arrived = jnp.take(normed, table_rows, axis=0, mode='fill', fill_value=0)
        gate_pre = blocked_product(arrived, gate_weight)
        up_pre = blocked_product(arrived, up_weight)
        hidden = (jax.nn.silu(gate_pre) * up_pre).astype(jnp.bfloat16)
        expert_out = jnp.dot(hidden, down_weight, preferred_element_type=jnp.float32).astype(jnp.bfloat16)
        totals = totals.at[table_rows].add(table_weights[:, None] * expert_out.astype(jnp.float32), mode='drop')
        return (totals, None)
    routed, _ = lax.scan(expert_step, jnp.zeros((TOKENS, D), jnp.float32), (token_table, weight_table, expert_gate, expert_up, expert_down))
    shared_gate_pre = blocked_product(normed, shared_gate)
    shared_up_pre = blocked_product(normed, shared_up)
    shared_hidden = (jax.nn.silu(shared_gate_pre) * shared_up_pre).astype(jnp.bfloat16)
    shared_out = jnp.dot(shared_hidden, shared_down, preferred_element_type=jnp.float32).astype(jnp.bfloat16)
    mixture = routed + shared_out.astype(jnp.float32)
    return (mixture * inverse_norm(mixture)[:, None] * post_gain.astype(jnp.float32)).astype(jnp.bfloat16)
```

```python
import functools

import jax
import jax.numpy as jnp
from jax import lax
from jax.experimental import pallas as pl
from jax.experimental.pallas import tpu as pltpu
from jax.sharding import PartitionSpec as P

epsilon = 1e-06
f32 = jnp.float32
bf16 = jnp.bfloat16


def dot(a, b):
    return jnp.dot(a, b, preferred_element_type=f32)


def shift(value, axis, count, inner, outer_by, inner_by):
    outer = count // inner
    pairs = []
    for i in range(count):
        o, n = divmod(i, inner)
        pairs.append((i, ((o + outer_by) % outer) * inner + (n + inner_by) % inner))
    return lax.ppermute(value, axis, pairs)


def normalized(tokens, inv_row, gain_row):
    count = tokens.shape[0]
    inv = jnp.broadcast_to(inv_row, (128, count)).T[:, :1]
    return (tokens.astype(f32) * inv * gain_row).astype(bf16)


def expand_body(where, xs, meta, gain, gk, uk, gs, us, keep, send, normed, rows):
    blocks = len(xs)
    local = (meta.shape[1] - 1) // 2
    capacity = keep.shape[1] // blocks
    half = gk.shape[2]
    e = pl.program_id(0)

    @pl.when(e == 0)
    def _():
        for j in range(blocks):
            normed[j] = normalized(
                xs[j][...], meta[where[j], pl.ds(2 * local, 1), :], gain[...]
            )

    for j in range(blocks):
        slot = meta[where[j], pl.ds(e, 1), :]
        count = slot.shape[1]
        lines = lax.broadcasted_iota(jnp.int32, (capacity, count), 0).astype(f32)
        pick = (lines == slot).astype(f32).astype(bf16)
        rows[j * capacity : (j + 1) * capacity, :] = dot(pick, normed[j]).astype(bf16)
    copies = rows[...]
    keep[0, :, :half] = dot(copies, gk[0]).astype(bf16)
    keep[0, :, half:] = dot(copies, uk[0]).astype(bf16)
    send[0, :, :half] = dot(copies, gs[0]).astype(bf16)
    send[0, :, half:] = dot(copies, us[0]).astype(bf16)


def expand(where, xs, meta, gain, gate, up, capacity):
    blocks = len(xs)
    count, width = xs[0].shape
    local, _, hidden = gate.shape
    half = hidden // 2

    def body(where, *refs):
        expand_body(where, refs[:blocks], *refs[blocks:])

    own = pl.BlockSpec((1, width, half), lambda e, w: (e, 0, w[blocks]))
    other = pl.BlockSpec((1, width, half), lambda e, w: (e, 0, 1 - w[blocks]))
    out = pl.BlockSpec((1, blocks * capacity, 2 * half), lambda e, w: (e, 0, 0))
    shape = jax.ShapeDtypeStruct((local, blocks * capacity, 2 * half), bf16)
    return pl.pallas_call(
        body,
        grid_spec=pltpu.PrefetchScalarGridSpec(
            num_scalar_prefetch=1,
            grid=(local,),
            in_specs=[pl.BlockSpec((count, width), lambda e, w: (0, 0))] * blocks
            + [
                pl.BlockSpec(meta.shape, lambda e, w: (0, 0, 0)),
                pl.BlockSpec(gain.shape, lambda e, w: (0, 0)),
                own,
                own,
                other,
                other,
            ],
            out_specs=[out, out],
            scratch_shapes=[
                pltpu.VMEM((blocks, count, width), bf16),
                pltpu.VMEM((blocks * capacity, width), bf16),
            ],
        ),
        out_shape=[shape, shape],
        name="expand",
    )(where, *xs, meta, gain, gate, up, gate, up)


def shared_expand_body(where, x, inv, gain, gk, uk, gs, us, keep, send):
    half = gk.shape[1]
    normed = normalized(x[...], inv[...], gain[...])
    keep[:, :half] = dot(normed, gk[...]).astype(bf16)
    keep[:, half:] = dot(normed, uk[...]).astype(bf16)
    send[:, :half] = dot(normed, gs[...]).astype(bf16)
    send[:, half:] = dot(normed, us[...]).astype(bf16)


def shared_expand(core, x, inv, gain, gate, up):
    count, width = x.shape
    half = gate.shape[1] // 2
    own = pl.BlockSpec((width, half), lambda i, w: (0, w[0]))
    other = pl.BlockSpec((width, half), lambda i, w: (0, 1 - w[0]))
    whole = lambda shape: pl.BlockSpec(shape, lambda i, w: (0, 0))
    shape = jax.ShapeDtypeStruct((count, 2 * half), bf16)
    return pl.pallas_call(
        shared_expand_body,
        grid_spec=pltpu.PrefetchScalarGridSpec(
            num_scalar_prefetch=1,
            grid=(1,),
            in_specs=[whole(x.shape), whole(inv.shape), whole(gain.shape), own, own, other, other],
            out_specs=[whole(shape.shape)] * 2,
        ),
        out_shape=[shape, shape],
        name="shared_expand",
    )(core, x, inv, gain, gate, up, gate, up)


def contract_body(where, mine, theirs, meta, dm, dt, *rest, blocks):
    outs, (products, spread) = rest[:blocks], rest[blocks:]
    local = (meta.shape[1] - 1) // 2
    capacity = mine.shape[1] // blocks
    count = meta.shape[2]
    e = pl.program_id(0)
    product = (dot(mine[0], dm[0]) + dot(theirs[0], dt[0])).astype(bf16)
    for j in range(blocks):
        products[j, pl.ds(pl.multiple_of(e * capacity, capacity), capacity), :] = product[
            j * capacity : (j + 1) * capacity
        ]

    @pl.when(e == local - 1)
    def _():
        lanes = lax.broadcasted_iota(jnp.int32, (count, capacity), 1).astype(f32)
        for j in range(blocks):
            for n in range(local):
                slot = meta[where[j], n : n + 1, :]
                weight = meta[where[j], local + n : local + n + 1, :]
                slot = jnp.broadcast_to(slot, (128, count)).T[:, :capacity]
                weight = jnp.broadcast_to(weight, (128, count)).T[:, :capacity]
                spread[:, n * capacity : (n + 1) * capacity] = jnp.where(
                    lanes == slot, weight, 0.0
                ).astype(bf16)
            outs[j][...] = dot(spread[...], products[j]).astype(bf16)


def contract(where, mine, theirs, meta, down, blocks):
    local, rows, half = mine.shape
    capacity = rows // blocks
    width = down.shape[2]
    count = meta.shape[2]
    part = pl.BlockSpec((1, rows, half), lambda e, w: (e, 0, 0))
    return pl.pallas_call(
        functools.partial(contract_body, blocks=blocks),
        grid_spec=pltpu.PrefetchScalarGridSpec(
            num_scalar_prefetch=1,
            grid=(local,),
            in_specs=[
                part,
                part,
                pl.BlockSpec(meta.shape, lambda e, w: (0, 0, 0)),
                pl.BlockSpec((1, half, width), lambda e, w: (e, w[blocks], 0)),
                pl.BlockSpec((1, half, width), lambda e, w: (e, 1 - w[blocks], 0)),
            ],
            out_specs=[pl.BlockSpec((count, width), lambda e, w: (0, 0))] * blocks,
            scratch_shapes=[
                pltpu.VMEM((blocks, local * capacity, width), bf16),
                pltpu.VMEM((count, local * capacity), bf16),
            ],
        ),
        out_shape=[jax.ShapeDtypeStruct((count, width), bf16)] * blocks,
        name="contract",
    )(where, mine, theirs, meta, down, down)


def shared_contract_body(where, mine, theirs, dm, dt, out):
    out[...] = (dot(mine[...], dm[...]) + dot(theirs[...], dt[...])).astype(bf16)


def shared_contract(core, mine, theirs, down):
    count, half = mine.shape
    width = down.shape[1]
    whole = lambda shape: pl.BlockSpec(shape, lambda i, w: (0, 0))
    return pl.pallas_call(
        shared_contract_body,
        grid_spec=pltpu.PrefetchScalarGridSpec(
            num_scalar_prefetch=1,
            grid=(1,),
            in_specs=[
                whole(mine.shape),
                whole(mine.shape),
                pl.BlockSpec((half, width), lambda i, w: (w[0], 0)),
                pl.BlockSpec((half, width), lambda i, w: (1 - w[0], 0)),
            ],
            out_specs=whole((count, width)),
        ),
        out_shape=jax.ShapeDtypeStruct((count, width), bf16),
        name="shared_contract",
    )(core, mine, theirs, down, down)


def per_device(
    tokens,
    routes,
    route_weights,
    pre_gain,
    expert_gate,
    expert_up,
    expert_down,
    shared_gate,
    shared_up,
    shared_down,
    post_gain,
    *,
    sizes,
):
    groups, nx, parts = sizes
    nz = groups // nx
    cores = 2
    ny = parts // cores
    count, width = tokens.shape
    features = width * parts
    local = expert_gate.shape[0]
    fanout = routes.shape[1]
    capacity = 2 * count * fanout // (local * groups)
    place = lax.axis_index("ep")
    z, x = place // nx, place % nx
    core = lax.axis_index("tp") % cores
    core_arg = core.reshape(1).astype(jnp.int32)

    def over_z(v):
        return shift(v, "ep", groups, nx, 1, 0)

    def over_x(v, by):
        return shift(v, "ep", groups, nx, 0, by)

    def over_y(v, by):
        return shift(v, "tp", parts, cores, by, 0)

    def over_core(v):
        return shift(v, "tp", parts, cores, 0, 1)

    def total(v):
        pair = v + over_core(v)
        return sum([over_y(pair, k) for k in range(1, ny)], pair)

    planes = []
    current = tokens
    for s in range(nz):
        with jax.named_scope(f"gather_{s}"):
            planes.append([current] + [over_x(current, k) for k in range(1, nx)])
            if s < nz - 1:
                current = over_z(current)

    inputs = tokens.astype(f32)
    inv_pre = lax.rsqrt(total(jnp.sum(inputs * inputs, axis=1)) / features + epsilon)
    facts = jnp.concatenate(
        [routes.T.astype(f32), route_weights.T, inv_pre[None, :]], axis=0
    )
    facts = lax.all_gather(facts, "ep", axis=0, tiled=False)
    names = facts[:, None, :fanout, :]
    wanted = (place * local + jnp.arange(local, dtype=jnp.int32)).astype(f32)
    hit = names == wanted[None, :, None, None]
    weight = jnp.sum(jnp.where(hit, facts[:, None, fanout : 2 * fanout, :], 0.0), axis=2)
    chosen = jnp.any(hit, axis=2)
    before = (
        lax.broadcasted_iota(jnp.int32, (count, count), 0)
        < lax.broadcasted_iota(jnp.int32, (count, count), 1)
    ).astype(bf16)
    rank = dot(chosen.astype(bf16).reshape(groups * local, count), before)
    slot = jnp.where(chosen, rank.reshape(groups, local, count), -1.0)
    meta = jnp.concatenate([slot, weight, facts[:, 2 * fanout :, :]], axis=1)
    gain = pre_gain[None, :]

    def reduce_and_activate(keep, send):
        pair = (keep.astype(f32) + over_core(send).astype(f32)).astype(bf16)
        whole = pair.astype(f32)
        for k in range(1, ny):
            whole = whole + over_y(pair, k).astype(f32)
        half = keep.shape[-1] // 2
        mine = (jax.nn.silu(whole[..., :half]) * whole[..., half:]).astype(bf16)
        return mine, over_core(mine)

    with jax.named_scope("shared"):
        keep, send = shared_expand(core_arg, tokens, inv_pre[None, :], gain, shared_gate, shared_up)
        mine, theirs = reduce_and_activate(keep, send)
        shared_out = shared_contract(core_arg, mine, theirs, shared_down)

    moving = None
    for s in list(range(1, nz)) + [0]:
        with jax.named_scope(f"plane_{s}"):
            ids = [((z - s) % nz) * nx + (x - k) % nx for k in range(nx)] + [core]
            where = jnp.stack(ids).astype(jnp.int32)
            keep, send = expand(
                where, planes[s], meta, gain, expert_gate, expert_up, capacity
            )
            mine, theirs = reduce_and_activate(keep, send)
            outs = contract(where, mine, theirs, meta, expert_down, nx)
            summed = outs[0].astype(f32)
            for k in range(1, nx):
                summed = summed + over_x(outs[k], -k).astype(f32)
            if moving is not None:
                summed = summed + moving.astype(f32)
            if s != 0:
                moving = over_z(summed.astype(bf16))

    mixture = summed + shared_out.astype(f32)
    inv_post = lax.rsqrt(total(jnp.sum(mixture * mixture, axis=1)) / features + epsilon)
    return (mixture * inv_post[:, None] * post_gain).astype(bf16)


def solution(mesh):
    in_specs = (
        P("ep", "tp"),
        P("ep", None),
        P("ep", None),
        P("tp"),
        P("ep", "tp", None),
        P("ep", "tp", None),
        P("ep", None, "tp"),
        P("tp", None),
        P("tp", None),
        P(None, "tp"),
        P("tp"),
    )
    out_specs = P("ep", "tp")
    groups, parts = mesh.shape["ep"], mesh.shape["tp"]
    places = [getattr(d, "coords", None) for d in mesh.devices.ravel()]
    nx = len({c[0] for c in places}) if all(c is not None for c in places) else 2
    return jax.shard_map(
        functools.partial(per_device, sizes=(groups, nx, parts)),
        mesh=mesh,
        in_specs=in_specs,
        out_specs=out_specs,
        check_vma=False,
    )
```
